32 devices in a mesh: dp: 4 (over y, x), kv: 4 (over z), tp: 2 (over core).
Axes of the slice: x: 2, y: 2, z: 4, core: 2. Of those that a mesh axis runs over, the one named last changes fastest.
Arguments:
- tokens: bfloat16 [4096, 2048], P(('dp', 'kv'), 'tp'), parts along dimension 0, may hold values from -6 to 6
- query_weight: bfloat16 [2048, 1024], P(None, 'tp'), may hold values from -2 to 2
- key_weight: bfloat16 [2048, 1024], P(None, 'tp'), may hold values from -2 to 2
- value_weight: bfloat16 [2048, 1024], P(None, 'tp'), may hold values from -0.125 to 0.125
- out_weight: bfloat16 [1024, 2048], P(None, 'tp'), may hold values from -0.75 to 0.75
- chosen: int32 [128, 16], P(('dp', 'kv')), parts along dimension 0, may hold values from -1 to 31, as said below
Outputs:
- mixed: bfloat16 [4096, 2048], P(('dp', 'kv'), 'tp'), parts along dimension 0
The draws below stay inside these ranges and needn't reach their ends.
There are 4 independent parts, one for each index of `dp`. The reference program is written for one: setup_inputs(seed, part) draws one part's arguments, and reference() takes and returns one part's arrays. A program takes and returns all parts, laid end to end along the dimension named above; an argument that names none is the same for every part. Nothing has to cross between parts.
Inputs may be any that keep to these rules, and one draw needn't show every extreme that they name: Each row of chosen lists distinct key blocks no later than its own query block, followed or mixed with -1 for empty slots; the own block is always listed, and block 0 too. For the 8 query blocks of one index of kv (aligned runs of rows), the distinct listed key blocks that lie among the 8 blocks of any one other index number at most 3, and exactly 3 for the index just before.
All inputs are finite; a program needn't handle non-finite values.
Results may differ from the reference program's by a relative error of at most 0.0084.
Values may be sent and summed in bfloat16 or wider, within the bound.
A program may use at most 128 MiB of HBM per device.

```python
import jax
import jax.numpy as jnp
from jax import lax

D = 2048
HEADS = 16
HEAD_DIM = 64
BLOCK = 32
TOPK = 16
CAP = 3
HW = 1024
BLK_DEV = 8
LEN = 1024
NBLK = 32


def paired_weights(key):
    first_key, second_key = jax.random.split(jax.random.fold_in(key, 5), 2)
    fan_scale = D ** (-0.5)
    base_draw = jax.random.normal(first_key, (D, HW), jnp.float32)
    other_draw = jax.random.normal(second_key, (D, HW), jnp.float32)
    query_part = base_draw
    key_part = other_draw
    return (jnp.clip(query_part * fan_scale, -2.0, 2.0), jnp.clip(key_part * fan_scale, -2.0, 2.0))


def draw_query_weight(key, part):
    return paired_weights(key)[0].astype(jnp.bfloat16)


def draw_key_weight(key, part):
    return paired_weights(key)[1].astype(jnp.bfloat16)


def draw_chosen(key, part):
    devices = NBLK // BLK_DEV
    key_popular, key_pick, key_score = jax.random.split(jax.random.fold_in(key, 11), 3)
    block_ids = jnp.arange(NBLK, dtype=jnp.int32)
    owner = block_ids // BLK_DEV
    local_index = block_ids % BLK_DEV
    popular = (jax.random.randint(key_popular, (NBLK,), 0, 8) == 0).astype(jnp.int32)
    asker = jnp.arange(devices, dtype=jnp.int32)[:, None]
    pick_score = jax.random.randint(key_pick, (devices, NBLK), 0, 4096) + popular[None, :] * 8192
    forced = (owner[None, :] == asker - 1) & (local_index[None, :] == BLK_DEV - 1) | (block_ids[None, :] == 0)
    pick_score = jnp.where(forced, 16384, pick_score) * BLK_DEV + (BLK_DEV - 1 - local_index)[None, :]
    pick_grid = pick_score.reshape(devices, devices, BLK_DEV)
    rank_in = jnp.sum((pick_grid[..., None, :] > pick_grid[..., :, None]).astype(jnp.int32), axis=-1)
    holder_ids = jnp.arange(devices, dtype=jnp.int32)
    allowed = (rank_in < CAP) & (holder_ids[None, :, None] < asker[:, :, None])
    allowed = allowed.reshape(devices, NBLK)
    query_block = block_ids[:, None]
    key_block = block_ids[None, :]
    query_owner = query_block // BLK_DEV
    local_ok = (key_block // BLK_DEV == query_owner) & (key_block <= query_block)
    remote_ok = allowed[query_owner[:, 0]]
    valid = local_ok | remote_ok
    mandatory = (key_block == query_block) | remote_ok & (key_block // BLK_DEV == query_owner - 1)
    mandatory = mandatory | (key_block == 0) & valid
    noise = jax.random.randint(key_score, (NBLK, NBLK), 0, 4096) + popular[None, :] * 4096
    score_int = jnp.where(mandatory, 16384, noise)
    score_int = jnp.where(valid, score_int * NBLK + key_block, -1)
    top_values, top_index = lax.top_k(score_int, TOPK)
    return jnp.where(top_values >= 0, top_index, -1).astype(jnp.int32)


def levels(own_key, shape, cuts, low, top_value):
    loudness, own = 1.0, jax.random.fold_in(own_key, 6)
    for position, parts in cuts:
        steps = jnp.exp(jax.random.uniform(jax.random.fold_in(own, position), (parts,), jnp.float32, low / len(cuts), top_value / len(cuts)))
        loudness = loudness * jnp.repeat(steps, shape[position] // parts).reshape([-1 if axis == position else 1 for axis in range(len(shape))])
    return loudness


def centred(rng, shape, spread, reach, cuts=(), kind=jnp.bfloat16):
    result = spread * jax.random.normal(rng, shape, jnp.float32)
    if cuts:
        result = result * levels(rng, shape, cuts, -0.22, 0.18)
    return jnp.clip(result, -reach, reach).astype(kind)


def setup_inputs(seed: int = 0, part: int = 0) -> dict:
    arg_keys = jax.random.split(jax.random.key(seed), 7)
    part_keys = jax.random.split(jax.random.fold_in(arg_keys[6], part), 7)
    return {
        "tokens": centred(part_keys[0], (LEN, D), 1.0, 6.0, ((0, 4), (1, 2))),
        "query_weight": draw_query_weight(jax.random.fold_in(arg_keys[6], 71), part),
        "key_weight": draw_key_weight(jax.random.fold_in(arg_keys[6], 71), part),
        "value_weight": centred(arg_keys[3], (D, HW), D ** -0.5, 0.125, ((1, 2),)),
        "out_weight": centred(arg_keys[4], (HW, D), (HW // 16) ** -0.5, 0.75, ((1, 2),)),
        "chosen": draw_chosen(jax.random.fold_in(jax.random.fold_in(arg_keys[6], part), 71), part),
    }


rotary_base = 500000.0
masked_score = -1e30


def rotate(heads_in, positions):
    half_dim = heads_in.shape[-1] // 2
    inverse = 1.0 / (rotary_base ** (jnp.arange(half_dim, dtype=jnp.float32) / half_dim))
    angles = positions.astype(jnp.float32)[:, None] * inverse[None, :]
    cosine = jnp.cos(angles)[:, None, :]
    sine_part = jnp.sin(angles)[:, None, :]
    first_half = heads_in[..., :half_dim]
    second_half = heads_in[..., half_dim:]
    return jnp.concatenate([first_half * cosine - second_half * sine_part,
                            first_half * sine_part + second_half * cosine], axis=-1)


def reference(tokens, query_weight, key_weight, value_weight, out_weight, chosen):
    length = tokens.shape[0]
    positions = jnp.arange(length, dtype=jnp.int32)
    heads_shape = (length, HEADS, HEAD_DIM)
    query_proj = rotate(jnp.dot(tokens, query_weight, preferred_element_type=jnp.float32).reshape(heads_shape),
                        positions).astype(jnp.bfloat16)
    key_proj = rotate(jnp.dot(tokens, key_weight, preferred_element_type=jnp.float32).reshape(heads_shape),
                      positions).astype(jnp.bfloat16)
    value_proj = jnp.dot(tokens, value_weight, preferred_element_type=jnp.float32).astype(jnp.bfloat16).reshape(heads_shape)
    blocks = length // BLOCK
    key_blocks = key_proj.reshape(blocks, BLOCK, HEADS, HEAD_DIM)
    value_blocks = value_proj.reshape(blocks, BLOCK, HEADS, HEAD_DIM)
    query_blocks = query_proj.reshape(blocks, BLOCK, HEADS, HEAD_DIM)
    score_scale = HEAD_DIM ** -0.5

    def one_block(inputs):
        query_block, listed, block_index = inputs
        safe_index = jnp.maximum(listed, 0).astype(jnp.int32)
        keys_sel = key_blocks[safe_index].reshape(TOPK * BLOCK, HEADS, HEAD_DIM).astype(jnp.float32)
        values_sel = value_blocks[safe_index].reshape(TOPK * BLOCK, HEADS, HEAD_DIM).astype(jnp.float32)
        key_pos = (safe_index[:, None] * BLOCK + jnp.arange(BLOCK, dtype=jnp.int32)[None, :]).reshape(-1)
        key_valid = jnp.repeat(listed >= 0, BLOCK)
        query_pos = block_index * BLOCK + jnp.arange(BLOCK, dtype=jnp.int32)
        allowed = key_valid[None, :] & (key_pos[None, :] <= query_pos[:, None])
        scores = jnp.einsum("qhd,khd->hqk", query_block.astype(jnp.float32), keys_sel) * score_scale
        scores = jnp.where(allowed[None], scores, masked_score)
        peak_row = jnp.max(scores, axis=2, keepdims=True)
        weights = jnp.where(allowed[None], jnp.exp(scores - peak_row), 0.0)
        denominator = jnp.sum(weights, axis=2)
        weight_low = lax.optimization_barrier(weights.astype(jnp.bfloat16))
        summed = jnp.einsum("hqk,khd->qhd", weight_low.astype(jnp.float32), values_sel)
        return (summed / denominator.T[:, :, None]).astype(jnp.bfloat16)

    attended = lax.map(one_block, (query_blocks, chosen, jnp.arange(blocks, dtype=jnp.int32)))
    attended = attended.reshape(length, HEADS * HEAD_DIM)
    return jnp.dot(attended, out_weight, preferred_element_type=jnp.float32).astype(jnp.bfloat16)
```

```python
import functools

import jax
import jax.numpy as jnp
import numpy as np
from jax import lax
from jax.experimental import pallas as pl
from jax.experimental.pallas import tpu as pltpu
from jax.sharding import PartitionSpec as P

HEAD_DIM = 64
BLOCK = 32
CAP = 3
LANES = 128
ROTARY_BASE = 500000.0
MASKED = -1e30
MESH = pl.DeviceIdType.MESH
F32 = jnp.float32
BF16 = jnp.bfloat16


def rotary_tables(rows, devices):
    half = HEAD_DIM // 2
    inverse = (1.0 / ROTARY_BASE ** (np.arange(half, dtype=np.float64) / half))
    lanes = np.tile(inverse, LANES // half)[None, :]
    row_angle = np.arange(rows, dtype=np.float64)[:, None] * lanes
    base_angle = (np.arange(devices, dtype=np.float64) * rows)[:, None] * lanes
    pack = lambda a: np.concatenate([np.cos(a), np.sin(a)], axis=1).astype(np.float32)
    return pack(row_angle), pack(base_angle)


def listed_columns(chosen, holder, rows):
    blocks = rows // BLOCK
    ids = holder * blocks + lax.broadcasted_iota(jnp.int32, (blocks, rows), 1) // BLOCK
    hit = jnp.zeros((blocks, rows), F32)
    for slot in range(chosen.shape[1]):
        hit = jnp.where(chosen[:, slot : slot + 1] == ids, 1.0, hit)
    return hit


def selection(hit, earlier):
    blocks, rows = hit.shape
    need = jnp.broadcast_to(jnp.max(hit, axis=0, keepdims=True), hit.shape)
    rank = jnp.dot(need.astype(BF16), earlier, preferred_element_type=F32)
    shape = (CAP * BLOCK, rows)
    slot_row = lax.broadcasted_iota(jnp.int32, shape, 0)
    column = lax.broadcasted_iota(jnp.int32, shape, 1)
    wanted = (slot_row // BLOCK).astype(F32)
    place = jnp.where(need[:1] > 0.5, rank[:1], -1.0)
    same = (slot_row % BLOCK) == (column % BLOCK)
    return jnp.where(same & (place == wanted), 1.0, 0.0).astype(BF16)


def layer(
    devices,
    chosen_ref, base_ref, row_hbm, tok_hbm, wq_hbm, wk_hbm, wv_hbm, wo_hbm,
    out_ref,
    tab, tok_own, tok_peer, wq, wk, wv, wo, q_acc, k_acc, v_acc, k_own, v_own, q2,
    lists, k_send, v_send, k_recv, v_recv, peak, total, summed, att_own, att_peer,
    load_sem, tok_sem, att_sem, list_send, list_recv, key_send, key_recv,
):
    me = lax.axis_index("kv")
    core = lax.axis_index("tp")
    rows, half = tok_own.shape
    head_width = k_own.shape[1]
    pairs = head_width // LANES
    picked = CAP * BLOCK
    other = 1 - core

    loads = [
        pltpu.make_async_copy(src, dst, load_sem.at[i])
        for i, (src, dst) in enumerate(
            ((tok_hbm, tok_own), (wk_hbm, wk), (row_hbm, tab), (wv_hbm, wv), (wq_hbm, wq), (wo_hbm, wo))
        )
    ]
    for load in loads:
        load.start()
    tok_load, wk_load, tab_load, wv_load, wq_load, wo_load = loads

    barrier = pltpu.get_barrier_semaphore()
    pl.semaphore_signal(barrier, inc=1, device_id={"tp": other}, device_id_type=MESH)

    def greet(d, _):
        pl.semaphore_signal(
            barrier, inc=1, device_id={"kv": lax.rem(me + d, devices)}, device_id_type=MESH
        )
        return 0

    lax.fori_loop(1, devices, greet, 0)

    own_half = pl.ds(pl.multiple_of(core * half, half), half)
    peer_half = pl.ds(pl.multiple_of(other * half, half), half)

    tok_load.wait()
    wk_load.wait()
    k_acc[...] = jnp.dot(tok_own[...], wk[own_half, :], preferred_element_type=F32)

    pl.semaphore_wait(barrier, devices)
    tok_copy = pltpu.make_async_remote_copy(
        src_ref=tok_own, dst_ref=tok_peer, send_sem=tok_sem.at[0], recv_sem=tok_sem.at[1],
        device_id={"tp": other}, device_id_type=MESH,
    )
    tok_copy.start()

    def list_copy(d, target):
        return pltpu.make_async_remote_copy(
            src_ref=chosen_ref, dst_ref=lists.at[d], send_sem=list_send.at[d],
            recv_sem=list_recv.at[d], device_id={"kv": target}, device_id_type=MESH,
        )

    def send_list(d, _):
        list_copy(d, me - d).start()
        return 0

    lax.fori_loop(1, me + 1, send_list, 0)

    wv_load.wait()
    v_acc[...] = jnp.dot(tok_own[...], wv[own_half, :], preferred_element_type=F32)
    wq_load.wait()
    q_acc[...] = jnp.dot(tok_own[...], wq[own_half, :], preferred_element_type=F32)

    tab_load.wait()
    lane = lax.broadcasted_iota(jnp.int32, (rows, LANES), 1)
    first = (lane % HEAD_DIM) < HEAD_DIM // 2
    base = base_ref[pl.ds(me, 1), :]
    row_cos, row_sin = tab[:, :LANES], tab[:, LANES:]
    base_cos, base_sin = base[:, :LANES], base[:, LANES:]
    cosine = row_cos * base_cos - row_sin * base_sin
    sine = row_sin * base_cos + row_cos * base_sin
    sine = jnp.where(first, -sine, sine)
    tab[:, :LANES] = cosine
    tab[:, LANES:] = sine

    def rotated(x):
        swapped = jnp.where(
            first,
            pltpu.roll(x, LANES - HEAD_DIM // 2, axis=1),
            pltpu.roll(x, HEAD_DIM // 2, axis=1),
        )
        return x * tab[:, :LANES] + swapped * tab[:, LANES:]

    row_i = lax.broadcasted_iota(jnp.int32, (rows, rows), 0)
    col_i = lax.broadcasted_iota(jnp.int32, (rows, rows), 1)
    earlier = jnp.where((row_i % BLOCK == 0) & (row_i // BLOCK < col_i // BLOCK), 1.0, 0.0).astype(BF16)

    tok_copy.wait_recv()
    k_full = k_acc[...] + jnp.dot(tok_peer[...], wk[peer_half, :], preferred_element_type=F32)
    for i in range(pairs):
        tile = slice(i * LANES, (i + 1) * LANES)
        k_own[:, tile] = rotated(k_full[:, tile]).astype(BF16)

    def row_copy(kind, d, target):
        source, landing = ((k_send, k_recv), (v_send, v_recv))[kind]
        return pltpu.make_async_remote_copy(
            src_ref=source.at[d], dst_ref=landing.at[d], send_sem=key_send.at[kind, d],
            recv_sem=key_recv.at[kind, d], device_id={"kv": target}, device_id_type=MESH,
        )

    def send_keys(step, _):
        d = devices - 1 - me - step
        list_copy(d, me).wait_recv()
        pick = selection(listed_columns(lists[d], me, rows), earlier)
        k_send[d] = jnp.dot(pick, k_own[...], preferred_element_type=F32).astype(BF16)
        row_copy(0, d, me + d).start()
        return 0

    lax.fori_loop(0, devices - 1 - me, send_keys, 0)

    v_own[...] = (
        v_acc[...] + jnp.dot(tok_peer[...], wv[peer_half, :], preferred_element_type=F32)
    ).astype(BF16)

    def send_values(step, _):
        d = devices - 1 - me - step
        pick = selection(listed_columns(lists[d], me, rows), earlier)
        v_send[d] = jnp.dot(pick, v_own[...], preferred_element_type=F32).astype(BF16)
        row_copy(1, d, me + d).start()
        return 0

    lax.fori_loop(0, devices - 1 - me, send_values, 0)

    q_full = q_acc[...] + jnp.dot(tok_peer[...], wq[peer_half, :], preferred_element_type=F32)
    for i in range(pairs):
        tile = slice(i * LANES, (i + 1) * LANES)
        q = rotated(q_full[:, tile]).astype(BF16).astype(F32) * (HEAD_DIM**-0.5)
        q2[i, :rows, :] = jnp.where(lane < HEAD_DIM, q, 0.0).astype(BF16)
        q2[i, rows:, :] = jnp.where(lane < HEAD_DIM, 0.0, q).astype(BF16)

    chosen = chosen_ref[...]

    def spread(hit):
        keys = hit.shape[1]
        blocks = hit.shape[0]
        wide = jnp.broadcast_to(hit[:, None, :], (blocks, BLOCK, keys))
        return wide.reshape(blocks * BLOCK, keys)

    def scores_of(i, keys):
        return lax.dot_general(
            q2[i], keys, (((1,), (1,)), ((), ())), preferred_element_type=F32
        )

    listed = spread(listed_columns(chosen, me, rows))
    bias = jnp.where((listed > 0.5) & (col_i <= row_i), 0.0, MASKED)
    bias = jnp.concatenate([bias, bias], axis=0)
    for i in range(pairs):
        tile = slice(i * LANES, (i + 1) * LANES)
        scores = scores_of(i, k_own[:, tile]) + bias
        top = jnp.max(scores, axis=1, keepdims=True)
        weights = jnp.exp(scores - top)
        peak[i] = top
        total[i] = jnp.sum(weights, axis=1, keepdims=True)
        summed[i] = jnp.dot(weights.astype(BF16), v_own[:, tile], preferred_element_type=F32)

    def attend(d, _):
        hit = listed_columns(chosen, me - d, rows)
        pick = selection(hit, earlier)
        got = lax.dot_general(
            hit.astype(BF16), pick, (((1,), (1,)), ((), ())), preferred_element_type=F32
        )
        far = jnp.where(spread(got) > 0.5, 0.0, MASKED)
        far = jnp.concatenate([far, far], axis=0)
        row_copy(0, d, me).wait_recv()
        row_copy(1, d, me).wait_recv()
        for i in range(pairs):
            tile = slice(i * LANES, (i + 1) * LANES)
            scores = scores_of(i, k_recv[d, :, tile]) + far
            old = peak[i]
            top = jnp.maximum(old, jnp.max(scores, axis=1, keepdims=True))
            factor = jnp.exp(old - top)
            weights = jnp.exp(scores - top)
            peak[i] = top
            total[i] = total[i] * factor + jnp.sum(weights, axis=1, keepdims=True)
            summed[i] = summed[i] * factor + jnp.dot(
                weights.astype(BF16), v_recv[d, :, tile], preferred_element_type=F32
            )
        return 0

    lax.fori_loop(1, me + 1, attend, 0)

    for i in range(pairs):
        tile = slice(i * LANES, (i + 1) * LANES)
        ratio = summed[i] / total[i]
        att_own[:, tile] = jnp.where(lane < HEAD_DIM, ratio[:rows], ratio[rows:]).astype(BF16)
    att_copy = pltpu.make_async_remote_copy(
        src_ref=att_own, dst_ref=att_peer, send_sem=att_sem.at[0], recv_sem=att_sem.at[1],
        device_id={"tp": other}, device_id_type=MESH,
    )
    att_copy.start()
    wo_load.wait()
    own_rows = pl.ds(pl.multiple_of(core * head_width, head_width), head_width)
    peer_rows = pl.ds(pl.multiple_of(other * head_width, head_width), head_width)
    mixed = jnp.dot(att_own[...], wo[own_rows, :], preferred_element_type=F32)
    att_copy.wait_recv()
    mixed = mixed + jnp.dot(att_peer[...], wo[peer_rows, :], preferred_element_type=F32)
    out_ref[...] = mixed.astype(BF16)

    att_copy.wait_send()
    tok_copy.wait_send()

    def drain_list(d, _):
        list_copy(d, me - d).wait_send()
        return 0

    lax.fori_loop(1, me + 1, drain_list, 0)

    def drain_rows(d, _):
        row_copy(0, d, me + d).wait_send()
        row_copy(1, d, me + d).wait_send()
        return 0

    lax.fori_loop(1, devices - me, drain_rows, 0)


def on_device(devices, tokens, query_weight, key_weight, value_weight, out_weight, chosen):
    rows, half = tokens.shape
    width, head_width = query_weight.shape
    pairs = head_width // LANES
    picked = CAP * BLOCK
    row_table, base_table = rotary_tables(rows, devices)
    vmem = pl.BlockSpec(memory_space=pltpu.VMEM)
    anywhere = pl.BlockSpec(memory_space=pl.ANY)
    dma = pltpu.SemaphoreType.DMA
    return pl.pallas_call(
        functools.partial(layer, devices),
        out_shape=jax.ShapeDtypeStruct((rows, out_weight.shape[1]), BF16),
        in_specs=[vmem, vmem] + [anywhere] * 6,
        out_specs=vmem,
        scratch_shapes=[
            pltpu.VMEM((rows, 2 * LANES), F32),
            pltpu.VMEM((rows, half), BF16),
            pltpu.VMEM((rows, half), BF16),
            pltpu.VMEM((width, head_width), BF16),
            pltpu.VMEM((width, head_width), BF16),
            pltpu.VMEM((width, head_width), BF16),
            pltpu.VMEM(out_weight.shape, BF16),
            pltpu.VMEM((rows, head_width), F32),
            pltpu.VMEM((rows, head_width), F32),
            pltpu.VMEM((rows, head_width), F32),
            pltpu.VMEM((rows, head_width), BF16),
            pltpu.VMEM((rows, head_width), BF16),
            pltpu.VMEM((pairs, 2 * rows, LANES), BF16),
            pltpu.VMEM((devices,) + chosen.shape, jnp.int32),
            pltpu.VMEM((devices, picked, head_width), BF16),
            pltpu.VMEM((devices, picked, head_width), BF16),
            pltpu.VMEM((devices, picked, head_width), BF16),
            pltpu.VMEM((devices, picked, head_width), BF16),
            pltpu.VMEM((pairs, 2 * rows, 1), F32),
            pltpu.VMEM((pairs, 2 * rows, 1), F32),
            pltpu.VMEM((pairs, 2 * rows, LANES), F32),
            pltpu.VMEM((rows, head_width), BF16),
            pltpu.VMEM((rows, head_width), BF16),
            dma((6,)),
            dma((2,)),
            dma((2,)),
            dma((devices,)),
            dma((devices,)),
            dma((2, devices)),
            dma((2, devices)),
        ],
        compiler_params=pltpu.CompilerParams(
            collective_id=0, has_side_effects=True, vmem_limit_bytes=60 * 1024 * 1024
        ),
        name="layer",
    )(
        chosen, jnp.asarray(base_table), jnp.asarray(row_table), tokens,
        query_weight, key_weight, value_weight, out_weight,
    )


def solution(mesh):
    placed = (
        P(("dp", "kv"), "tp"),
        P(None, "tp"),
        P(None, "tp"),
        P(None, "tp"),
        P(None, "tp"),
        P(("dp", "kv"), None),
    )
    return jax.shard_map(
        functools.partial(on_device, mesh.shape["kv"]),
        mesh=mesh, in_specs=placed, out_specs=P(("dp", "kv"), "tp"), check_vma=False,
    )
```

```python
import functools

import jax
import jax.numpy as jnp
import numpy as np
from jax import lax
from jax.experimental import pallas as pl
from jax.experimental.pallas import tpu as pltpu
from jax.sharding import PartitionSpec as P

HEAD_DIM = 64
BLOCK = 32
CAP = 3
LANES = 128
ROTARY_BASE = 500000.0
MASKED = -1e30
MESH = pl.DeviceIdType.MESH
F32 = jnp.float32
BF16 = jnp.bfloat16


def rotary_tables(rows, devices):
    half = HEAD_DIM // 2
    inverse = (1.0 / ROTARY_BASE ** (np.arange(half, dtype=np.float64) / half))
    lanes = np.tile(inverse, LANES // half)[None, :]
    row_angle = np.arange(rows, dtype=np.float64)[:, None] * lanes
    base_angle = (np.arange(devices, dtype=np.float64) * rows)[:, None] * lanes
    pack = lambda a: np.concatenate([np.cos(a), np.sin(a)], axis=1).astype(np.float32)
    return pack(row_angle), pack(base_angle)


def listed_columns(chosen, holder, rows):
    blocks = rows // BLOCK
    ids = holder * blocks + lax.broadcasted_iota(jnp.int32, (blocks, rows), 1) // BLOCK
    hit = jnp.zeros((blocks, rows), F32)
    for slot in range(chosen.shape[1]):
        hit = jnp.where(chosen[:, slot : slot + 1] == ids, 1.0, hit)
    return hit


def selection(hit, earlier):
    blocks, rows = hit.shape
    need = jnp.broadcast_to(jnp.max(hit, axis=0, keepdims=True), hit.shape)
    rank = jnp.dot(need.astype(BF16), earlier, preferred_element_type=F32)
    shape = (CAP * BLOCK, rows)
    slot_row = lax.broadcasted_iota(jnp.int32, shape, 0)
    column = lax.broadcasted_iota(jnp.int32, shape, 1)
    wanted = (slot_row // BLOCK).astype(F32)
    place = jnp.where(need[:1] > 0.5, rank[:1], -1.0)
    same = (slot_row % BLOCK) == (column % BLOCK)
    return jnp.where(same & (place == wanted), 1.0, 0.0).astype(BF16)


def layer(
    devices,
    chosen_hbm, base_hbm, row_hbm, tok_hbm, wq_hbm, wk_hbm, wv_hbm, wo_hbm,
    out_ref,
    chosen_ref, base_ref, tab, tok_own, tok_peer, wq, wk, wv, wo, q_acc, k_acc, v_acc, k_own, v_own, q2,
    lists, picks, k_send, v_send, k_recv, v_recv, peak, total, summed, weigh, att_own, att_peer,
    load_sem, tok_sem, att_sem, list_send, list_recv, key_send, key_recv, root_send, root_recv,
):
    me = lax.axis_index("kv")
    core = lax.axis_index("tp")
    rows, half = tok_own.shape
    head_width = k_own.shape[1]
    pairs = head_width // LANES
    picked = CAP * BLOCK
    other = 1 - core

    loads = [
        pltpu.make_async_copy(src, dst, load_sem.at[i])
        for i, (src, dst) in enumerate(
            ((chosen_hbm, chosen_ref), (base_hbm, base_ref), (tok_hbm, tok_own), (wk_hbm, wk), (row_hbm, tab), (wv_hbm, wv), (wq_hbm, wq), (wo_hbm, wo))
        )
    ]
    for load in loads:
        load.start()
    chosen_load, base_load, tok_load, wk_load, tab_load, wv_load, wq_load, wo_load = loads

    barrier = pltpu.get_barrier_semaphore()
    pl.semaphore_signal(barrier, inc=1, device_id={"tp": other}, device_id_type=MESH)

    def greet(d, _):
        pl.semaphore_signal(
            barrier, inc=1, device_id={"kv": lax.rem(me + d, devices)}, device_id_type=MESH
        )
        return 0

    lax.fori_loop(1, devices, greet, 0)

    own_half = pl.ds(pl.multiple_of(core * half, half), half)
    peer_half = pl.ds(pl.multiple_of(other * half, half), half)

    tok_load.wait()
    wk_load.wait()
    k_acc[...] = jnp.dot(tok_own[...], wk[own_half, :], preferred_element_type=F32)

    pl.semaphore_wait(barrier, devices)

    def list_copy(d, target):
        return pltpu.make_async_remote_copy(
            src_ref=chosen_ref, dst_ref=lists.at[d], send_sem=list_send.at[d],
            recv_sem=list_recv.at[d], device_id={"kv": target}, device_id_type=MESH,
        )

    def send_list(d, _):
        list_copy(d, me - d).start()
        return 0

    chosen_load.wait()
    lax.fori_loop(1, me + 1, send_list, 0)
    tok_copy = pltpu.make_async_remote_copy(
        src_ref=tok_own, dst_ref=tok_peer, send_sem=tok_sem.at[0], recv_sem=tok_sem.at[1],
        device_id={"tp": other}, device_id_type=MESH,
    )
    tok_copy.start()

    wv_load.wait()
    v_acc[...] = jnp.dot(tok_own[...], wv[own_half, :], preferred_element_type=F32)
    wq_load.wait()
    q_acc[...] = jnp.dot(tok_own[...], wq[own_half, :], preferred_element_type=F32)

    tab_load.wait()
    base_load.wait()
    lane = lax.broadcasted_iota(jnp.int32, (rows, LANES), 1)
    first = (lane % HEAD_DIM) < HEAD_DIM // 2
    base = base_ref[pl.ds(me, 1), :]
    row_cos, row_sin = tab[:, :LANES], tab[:, LANES:]
    base_cos, base_sin = base[:, :LANES], base[:, LANES:]
    cosine = row_cos * base_cos - row_sin * base_sin
    sine = row_sin * base_cos + row_cos * base_sin
    sine = jnp.where(first, -sine, sine)
    tab[:, :LANES] = cosine
    tab[:, LANES:] = sine

    def rotated(x):
        swapped = jnp.where(
            first,
            pltpu.roll(x, LANES - HEAD_DIM // 2, axis=1),
            pltpu.roll(x, HEAD_DIM // 2, axis=1),
        )
        return x * tab[:, :LANES] + swapped * tab[:, LANES:]

    row_i = lax.broadcasted_iota(jnp.int32, (rows, rows), 0)
    col_i = lax.broadcasted_iota(jnp.int32, (rows, rows), 1)
    earlier = jnp.where((row_i % BLOCK == 0) & (row_i // BLOCK < col_i // BLOCK), 1.0, 0.0).astype(BF16)

    tok_copy.wait_recv()
    k_full = k_acc[...] + jnp.dot(tok_peer[...], wk[peer_half, :], preferred_element_type=F32)
    for i in range(pairs):
        tile = slice(i * LANES, (i + 1) * LANES)
        k_own[:, tile] = rotated(k_full[:, tile]).astype(BF16)

    buffers = ((k_own, k_send, k_recv), (v_own, v_send, v_recv))

    def row_copy(kind, d, target, holder):
        _, source, landing = buffers[kind]

        def part(span):
            return pltpu.make_async_remote_copy(
                src_ref=source.at[d, span], dst_ref=landing.at[d, span],
                send_sem=key_send.at[kind, d], recv_sem=key_recv.at[kind, d],
                device_id={"kv": target}, device_id_type=MESH,
            )

        return part(slice(BLOCK, picked)), part(slice(0, picked)), holder == 0

    def each(copies, act):
        short, whole, is_short = copies
        pl.when(is_short)(lambda: act(short))
        pl.when(jnp.logical_not(is_short))(lambda: act(whole))

    def root_copy(kind, from_own):
        own, _, landing = buffers[kind]
        block = slice(0, BLOCK)
        source = own.at[block] if from_own else landing.at[me, block]
        return pltpu.make_async_remote_copy(
            src_ref=source, dst_ref=landing.at[lax.rem(me + 1, devices), block],
            send_sem=root_send.at[kind], recv_sem=root_recv.at[kind],
            device_id={"kv": lax.rem(me + 1, devices)}, device_id_type=MESH,
        )

    def root_arrival(kind):
        landing = buffers[kind][2]
        block = slice(0, BLOCK)
        return pltpu.make_async_remote_copy(
            src_ref=landing.at[me, block], dst_ref=landing.at[me, block],
            send_sem=root_send.at[kind], recv_sem=root_recv.at[kind],
            device_id={"kv": lax.rem(me + 1, devices)}, device_id_type=MESH,
        )

    @pl.when(me == 0)
    def _():
        root_copy(0, True).start()

    def send_keys(d, _):
        list_copy(d, me).wait_recv()
        pick = selection(listed_columns(lists[d], me, rows), earlier)
        picks[d] = pick
        k_send[d] = jnp.dot(pick, k_own[...], preferred_element_type=F32).astype(BF16)
        each(row_copy(0, d, me + d, me), lambda c: c.start())
        return 0

    lax.fori_loop(1, devices - me, send_keys, 0)

    v_own[...] = (
        v_acc[...] + jnp.dot(tok_peer[...], wv[peer_half, :], preferred_element_type=F32)
    ).astype(BF16)

    @pl.when(me == 0)
    def _():
        root_copy(1, True).start()

    def send_values(step, _):
        d = devices - 1 - me - step
        v_send[d] = jnp.dot(picks[d], v_own[...], preferred_element_type=F32).astype(BF16)
        each(row_copy(1, d, me + d, me), lambda c: c.start())
        return 0

    lax.fori_loop(0, devices - 1 - me, send_values, 0)

    q_full = q_acc[...] + jnp.dot(tok_peer[...], wq[peer_half, :], preferred_element_type=F32)
    for i in range(pairs):
        tile = slice(i * LANES, (i + 1) * LANES)
        q = rotated(q_full[:, tile]).astype(BF16).astype(F32) * (HEAD_DIM**-0.5)
        q2[i, :rows, :] = jnp.where(lane < HEAD_DIM, q, 0.0).astype(BF16)
        q2[i, rows:, :] = jnp.where(lane < HEAD_DIM, 0.0, q).astype(BF16)

    chosen = chosen_ref[...]

    def spread(hit):
        keys = hit.shape[1]
        blocks = hit.shape[0]
        wide = jnp.broadcast_to(hit[:, None, :], (blocks, BLOCK, keys))
        return wide.reshape(blocks * BLOCK, keys)

    def scores_of(i, keys):
        return lax.dot_general(
            q2[i], keys, (((1,), (1,)), ((), ())), preferred_element_type=F32
        )

    def relay(kind):
        @pl.when(me > 0)
        def _():
            root_arrival(kind).wait_recv()

            @pl.when(me < devices - 1)
            def _():
                root_copy(kind, False).start()

    relay(0)
    listed = spread(listed_columns(chosen, me, rows))
    bias = jnp.where((listed > 0.5) & (col_i <= row_i), 0.0, MASKED)
    bias = jnp.concatenate([bias, bias], axis=0)
    for i in range(pairs):
        tile = slice(i * LANES, (i + 1) * LANES)
        scores = scores_of(i, k_own[:, tile]) + bias
        top = jnp.max(scores, axis=1, keepdims=True)
        weights = jnp.exp(scores - top)
        peak[i] = top
        total[i] = jnp.sum(weights, axis=1, keepdims=True)
        summed[i] = jnp.dot(weights.astype(BF16), v_own[:, tile], preferred_element_type=F32)
    relay(1)

    def attend(step, _):
        d = jnp.where(me == devices - 1, step, me + 1 - step)
        hit = listed_columns(chosen, me - d, rows)
        pick = selection(hit, earlier)
        got = lax.dot_general(
            hit.astype(BF16), pick, (((1,), (1,)), ((), ())), preferred_element_type=F32
        )
        far = jnp.where(spread(got) > 0.5, 0.0, MASKED)
        far = jnp.concatenate([far, far], axis=0)
        each(row_copy(0, d, me, me - d), lambda c: c.wait_recv())
        for i in range(pairs):
            tile = slice(i * LANES, (i + 1) * LANES)
            scores = scores_of(i, k_recv[d, :, tile]) + far
            old = peak[i]
            top = jnp.maximum(old, jnp.max(scores, axis=1, keepdims=True))
            factor = jnp.exp(old - top)
            weights = jnp.exp(scores - top)
            peak[i] = top
            total[i] = total[i] * factor + jnp.sum(weights, axis=1, keepdims=True)
            summed[i] = summed[i] * factor
            weigh[i] = weights.astype(BF16)
        each(row_copy(1, d, me, me - d), lambda c: c.wait_recv())
        for i in range(pairs):
            tile = slice(i * LANES, (i + 1) * LANES)
            summed[i] += jnp.dot(weigh[i], v_recv[d, :, tile], preferred_element_type=F32)
        return 0

    lax.fori_loop(1, me + 1, attend, 0)

    att_copies = []
    for i in range(pairs):
        ratio = summed[i] / total[i]
        att_own[i] = jnp.where(lane < HEAD_DIM, ratio[:rows], ratio[rows:]).astype(BF16)
        att_copies.append(
            pltpu.make_async_remote_copy(
                src_ref=att_own.at[i], dst_ref=att_peer.at[i], send_sem=att_sem.at[0, i],
                recv_sem=att_sem.at[1, i], device_id={"tp": other}, device_id_type=MESH,
            )
        )
        att_copies[-1].start()
    wo_load.wait()
    own_rows = pl.ds(pl.multiple_of(core * head_width, head_width), head_width)
    peer_rows = pl.ds(pl.multiple_of(other * head_width, head_width), head_width)
    joined = lambda ref: jnp.concatenate([ref[i] for i in range(pairs)], axis=1)
    mixed = jnp.dot(joined(att_own), wo[own_rows, :], preferred_element_type=F32)
    for copy in att_copies:
        copy.wait_recv()
    mixed = mixed + jnp.dot(joined(att_peer), wo[peer_rows, :], preferred_element_type=F32)
    out_ref[...] = mixed.astype(BF16)

    for copy in att_copies:
        copy.wait_send()
    tok_copy.wait_send()

    def drain_list(d, _):
        list_copy(d, me - d).wait_send()
        return 0

    lax.fori_loop(1, me + 1, drain_list, 0)

    def drain_rows(d, _):
        each(row_copy(0, d, me + d, me), lambda c: c.wait_send())
        each(row_copy(1, d, me + d, me), lambda c: c.wait_send())
        return 0

    lax.fori_loop(1, devices - me, drain_rows, 0)

    @pl.when(me < devices - 1)
    def _():
        for kind in range(2):
            root_copy(kind, True).wait_send()


def on_device(devices, tokens, query_weight, key_weight, value_weight, out_weight, chosen):
    rows, half = tokens.shape
    width, head_width = query_weight.shape
    pairs = head_width // LANES
    picked = CAP * BLOCK
    row_table, base_table = rotary_tables(rows, devices)
    vmem = pl.BlockSpec(memory_space=pltpu.VMEM)
    anywhere = pl.BlockSpec(memory_space=pl.ANY)
    dma = pltpu.SemaphoreType.DMA
    return pl.pallas_call(
        functools.partial(layer, devices),
        out_shape=jax.ShapeDtypeStruct((rows, out_weight.shape[1]), BF16),
        in_specs=[anywhere] * 8,
        out_specs=vmem,
        scratch_shapes=[
            pltpu.VMEM(chosen.shape, jnp.int32),
            pltpu.VMEM(base_table.shape, F32),
            pltpu.VMEM((rows, 2 * LANES), F32),
            pltpu.VMEM((rows, half), BF16),
            pltpu.VMEM((rows, half), BF16),
            pltpu.VMEM((width, head_width), BF16),
            pltpu.VMEM((width, head_width), BF16),
            pltpu.VMEM((width, head_width), BF16),
            pltpu.VMEM(out_weight.shape, BF16),
            pltpu.VMEM((rows, head_width), F32),
            pltpu.VMEM((rows, head_width), F32),
            pltpu.VMEM((rows, head_width), F32),
            pltpu.VMEM((rows, head_width), BF16),
            pltpu.VMEM((rows, head_width), BF16),
            pltpu.VMEM((pairs, 2 * rows, LANES), BF16),
            pltpu.VMEM((devices,) + chosen.shape, jnp.int32),
            pltpu.VMEM((devices, picked, rows), BF16),
            pltpu.VMEM((devices, picked, head_width), BF16),
            pltpu.VMEM((devices, picked, head_width), BF16),
            pltpu.VMEM((devices, picked, head_width), BF16),
            pltpu.VMEM((devices, picked, head_width), BF16),
            pltpu.VMEM((pairs, 2 * rows, 1), F32),
            pltpu.VMEM((pairs, 2 * rows, 1), F32),
            pltpu.VMEM((pairs, 2 * rows, LANES), F32),
            pltpu.VMEM((pairs, 2 * rows, picked), BF16),
            pltpu.VMEM((pairs, rows, LANES), BF16),
            pltpu.VMEM((pairs, rows, LANES), BF16),
            dma((8,)),
            dma((2,)),
            dma((2, pairs)),
            dma((devices,)),
            dma((devices,)),
            dma((2, devices)),
            dma((2, devices)),
            dma((2,)),
            dma((2,)),
        ],
        compiler_params=pltpu.CompilerParams(
            collective_id=0, has_side_effects=True, vmem_limit_bytes=60 * 1024 * 1024
        ),
        name="layer",
    )(
        chosen, jnp.asarray(base_table), jnp.asarray(row_table), tokens,
        query_weight, key_weight, value_weight, out_weight,
    )


def solution(mesh):
    placed = (
        P(("dp", "kv"), "tp"),
        P(None, "tp"),
        P(None, "tp"),
        P(None, "tp"),
        P(None, "tp"),
        P(("dp", "kv"), None),
    )
    return jax.shard_map(
        functools.partial(on_device, mesh.shape["kv"]),
        mesh=mesh, in_specs=placed, out_specs=P(("dp", "kv"), "tp"), check_vma=False,
    )
```

```python
import functools

import jax
import jax.numpy as jnp
import numpy as np
from jax import lax
from jax.experimental import pallas as pl
from jax.experimental.pallas import tpu as pltpu
from jax.sharding import PartitionSpec as P

HEAD_DIM = 64
BLOCK = 32
CAP = 3
LANES = 128
ROTARY_BASE = 500000.0
MASKED = -1e30
MESH = pl.DeviceIdType.MESH
F32 = jnp.float32
BF16 = jnp.bfloat16


def rotary_tables(rows, devices):
    half = HEAD_DIM // 2
    inverse = (1.0 / ROTARY_BASE ** (np.arange(half, dtype=np.float64) / half))
    lanes = np.tile(inverse, LANES // half)[None, :]
    row_angle = np.arange(rows, dtype=np.float64)[:, None] * lanes
    base_angle = (np.arange(devices, dtype=np.float64) * rows)[:, None] * lanes
    pack = lambda a: np.concatenate([np.cos(a), np.sin(a)], axis=1).astype(np.float32)
    return pack(row_angle), pack(base_angle)


def listed_columns(chosen, holder, rows):
    blocks = rows // BLOCK
    ids = holder * blocks + lax.broadcasted_iota(jnp.int32, (blocks, rows), 1) // BLOCK
    hit = jnp.zeros((blocks, rows), F32)
    for slot in range(chosen.shape[1]):
        hit = jnp.where(chosen[:, slot : slot + 1] == ids, 1.0, hit)
    return hit


def selection(hit, earlier):
    blocks, rows = hit.shape
    need = jnp.broadcast_to(jnp.max(hit, axis=0, keepdims=True), hit.shape)
    rank = jnp.dot(need.astype(BF16), earlier, preferred_element_type=F32)
    shape = (CAP * BLOCK, rows)
    slot_row = lax.broadcasted_iota(jnp.int32, shape, 0)
    column = lax.broadcasted_iota(jnp.int32, shape, 1)
    wanted = (slot_row // BLOCK).astype(F32)
    place = jnp.where(need[:1] > 0.5, rank[:1], -1.0)
    same = (slot_row % BLOCK) == (column % BLOCK)
    return jnp.where(same & (place == wanted), 1.0, 0.0).astype(BF16)


def layer(
    devices,
    chosen_hbm, base_hbm, row_hbm, tok_hbm, wq_hbm, wk_hbm, wv_hbm, wo_hbm,
    out_ref,
    chosen_ref, base_ref, tab, tok_own, tok_peer, wq, wk, wv, wo, q_acc, k_acc, v_acc, k_own, v_own, q2,
    lists, picks, k_rows, v_rows, raw, widest, peak, total, summed, weigh, att_own, att_peer,
    load_sem, tok_sem, att_sem, list_send, list_recv, key_send, key_recv, root_send, root_recv,
):
    me = lax.axis_index("kv")
    core = lax.axis_index("tp")
    rows, half = tok_own.shape
    head_width = k_own.shape[1]
    pairs = head_width // LANES
    picked = CAP * BLOCK
    other = 1 - core

    loads = [
        pltpu.make_async_copy(src, dst, load_sem.at[i])
        for i, (src, dst) in enumerate(
            ((chosen_hbm, chosen_ref), (base_hbm, base_ref), (tok_hbm, tok_own), (wk_hbm, wk), (row_hbm, tab), (wv_hbm, wv), (wq_hbm, wq), (wo_hbm, wo))
        )
    ]
    for load in loads:
        load.start()
    chosen_load, base_load, tok_load, wk_load, tab_load, wv_load, wq_load, wo_load = loads

    barrier = pltpu.get_barrier_semaphore()
    pl.semaphore_signal(barrier, inc=1, device_id={"tp": other}, device_id_type=MESH)

    def greet(d, _):
        pl.semaphore_signal(
            barrier, inc=1, device_id={"kv": lax.rem(me + d, devices)}, device_id_type=MESH
        )
        return 0

    lax.fori_loop(1, devices, greet, 0)

    own_half = pl.ds(pl.multiple_of(core * half, half), half)
    peer_half = pl.ds(pl.multiple_of(other * half, half), half)

    tok_load.wait()
    wk_load.wait()
    k_acc[...] = jnp.dot(tok_own[...], wk[own_half, :], preferred_element_type=F32)

    pl.semaphore_wait(barrier, devices)

    def list_copy(d, target):
        return pltpu.make_async_remote_copy(
            src_ref=chosen_ref, dst_ref=lists.at[d], send_sem=list_send.at[d],
            recv_sem=list_recv.at[d], device_id={"kv": target}, device_id_type=MESH,
        )

    def send_list(d, _):
        list_copy(d, me - d).start()
        return 0

    chosen_load.wait()
    lax.fori_loop(1, me + 1, send_list, 0)
    tok_copy = pltpu.make_async_remote_copy(
        src_ref=tok_own, dst_ref=tok_peer, send_sem=tok_sem.at[0], recv_sem=tok_sem.at[1],
        device_id={"tp": other}, device_id_type=MESH,
    )
    tok_copy.start()

    wv_load.wait()
    v_acc[...] = jnp.dot(tok_own[...], wv[own_half, :], preferred_element_type=F32)
    wq_load.wait()
    q_acc[...] = jnp.dot(tok_own[...], wq[own_half, :], preferred_element_type=F32)

    tab_load.wait()
    base_load.wait()
    lane = lax.broadcasted_iota(jnp.int32, (rows, LANES), 1)
    first = (lane % HEAD_DIM) < HEAD_DIM // 2
    base = base_ref[pl.ds(me, 1), :]
    row_cos, row_sin = tab[:, :LANES], tab[:, LANES:]
    base_cos, base_sin = base[:, :LANES], base[:, LANES:]
    cosine = row_cos * base_cos - row_sin * base_sin
    sine = row_sin * base_cos + row_cos * base_sin
    sine = jnp.where(first, -sine, sine)
    tab[:, :LANES] = cosine
    tab[:, LANES:] = sine

    def rotated(x):
        swapped = jnp.where(
            first,
            pltpu.roll(x, LANES - HEAD_DIM // 2, axis=1),
            pltpu.roll(x, HEAD_DIM // 2, axis=1),
        )
        return x * tab[:, :LANES] + swapped * tab[:, LANES:]

    row_i = lax.broadcasted_iota(jnp.int32, (rows, rows), 0)
    col_i = lax.broadcasted_iota(jnp.int32, (rows, rows), 1)
    earlier = jnp.where((row_i % BLOCK == 0) & (row_i // BLOCK < col_i // BLOCK), 1.0, 0.0).astype(BF16)

    tok_copy.wait_recv()
    k_full = k_acc[...] + jnp.dot(tok_peer[...], wk[peer_half, :], preferred_element_type=F32)
    for i in range(pairs):
        tile = slice(i * LANES, (i + 1) * LANES)
        k_own[:, tile] = rotated(k_full[:, tile]).astype(BF16)

    buffers = ((k_own, k_rows), (v_own, v_rows))

    def row_copy(kind, d, target, holder):
        buffer = buffers[kind][1]

        def part(span):
            return pltpu.make_async_remote_copy(
                src_ref=buffer.at[lax.rem(me + d, devices), span], dst_ref=buffer.at[d, span],
                send_sem=key_send.at[kind, d], recv_sem=key_recv.at[kind, d],
                device_id={"kv": target}, device_id_type=MESH,
            )

        return part(slice(BLOCK, picked)), part(slice(0, picked)), holder == 0

    def each(copies, act):
        short, whole, is_short = copies
        pl.when(is_short)(lambda: act(short))
        pl.when(jnp.logical_not(is_short))(lambda: act(whole))

    def root_copy(kind, d):
        own, buffer = buffers[kind]
        block = slice(0, BLOCK)
        return pltpu.make_async_remote_copy(
            src_ref=own.at[block], dst_ref=buffer.at[d, block],
            send_sem=root_send.at[kind, d], recv_sem=root_recv.at[kind],
            device_id={"kv": lax.rem(d, devices)}, device_id_type=MESH,
        )

    def send_root(kind):
        @pl.when(me == 0)
        def _():
            def one(step, _):
                root_copy(kind, devices - 1 - step).start()
                return 0

            lax.fori_loop(0, devices - 1, one, 0)

    def arrived(kind, d):
        each(row_copy(kind, d, me, me - d), lambda c: c.wait_recv())

        @pl.when(d == me)
        def _():
            root_copy(kind, d).wait_recv()

    send_root(0)

    def send_keys(step, _):
        d = devices - 1 - me - step
        list_copy(d, me).wait_recv()
        pick = selection(listed_columns(lists[d], me, rows), earlier)
        picks[d] = pick
        k_rows[me + d] = jnp.dot(pick, k_own[...], preferred_element_type=F32).astype(BF16)
        each(row_copy(0, d, me + d, me), lambda c: c.start())
        return 0

    lax.fori_loop(0, devices - 1 - me, send_keys, 0)

    v_own[...] = (
        v_acc[...] + jnp.dot(tok_peer[...], wv[peer_half, :], preferred_element_type=F32)
    ).astype(BF16)

    send_root(1)

    def send_values(step, _):
        d = devices - 1 - me - step
        v_rows[me + d] = jnp.dot(picks[d], v_own[...], preferred_element_type=F32).astype(BF16)
        each(row_copy(1, d, me + d, me), lambda c: c.start())
        return 0

    lax.fori_loop(0, devices - 1 - me, send_values, 0)

    q_full = q_acc[...] + jnp.dot(tok_peer[...], wq[peer_half, :], preferred_element_type=F32)
    for i in range(pairs):
        tile = slice(i * LANES, (i + 1) * LANES)
        q = rotated(q_full[:, tile]).astype(BF16).astype(F32) * (HEAD_DIM**-0.5)
        q2[i, :rows, :] = jnp.where(lane < HEAD_DIM, q, 0.0).astype(BF16)
        q2[i, rows:, :] = jnp.where(lane < HEAD_DIM, 0.0, q).astype(BF16)

    chosen = chosen_ref[...]

    def spread(hit):
        keys = hit.shape[1]
        blocks = hit.shape[0]
        wide = jnp.broadcast_to(hit[:, None, :], (blocks, BLOCK, keys))
        return wide.reshape(blocks * BLOCK, keys)

    def scores_of(i, keys):
        return lax.dot_general(
            q2[i], keys, (((1,), (1,)), ((), ())), preferred_element_type=F32
        )

    def gauge(d, _):
        hit = listed_columns(chosen, me - d, rows)
        pick = selection(hit, earlier)
        got = lax.dot_general(
            hit.astype(BF16), pick, (((1,), (1,)), ((), ())), preferred_element_type=F32
        )
        far = jnp.where(spread(got) > 0.5, 0.0, MASKED)
        far = jnp.concatenate([far, far], axis=0)
        arrived(0, d)
        for i in range(pairs):
            tile = slice(i * LANES, (i + 1) * LANES)
            scores = scores_of(i, k_rows[d, :, tile]) + far
            raw[d - 1, i] = scores
            widest[i] = jnp.maximum(widest[i], scores)
        return 0

    listed = spread(listed_columns(chosen, me, rows))
    bias = jnp.where((listed > 0.5) & (col_i <= row_i), 0.0, MASKED)
    bias = jnp.concatenate([bias, bias], axis=0)
    for i in range(pairs):
        tile = slice(i * LANES, (i + 1) * LANES)
        scores = scores_of(i, k_own[:, tile]) + bias
        top = jnp.max(scores, axis=1, keepdims=True)
        weights = jnp.exp(scores - top)
        peak[i] = jnp.broadcast_to(top, peak.shape[1:])
        total[i] = sum(weights[:, j : j + LANES] for j in range(0, rows, LANES))
        summed[i] = jnp.dot(weights.astype(BF16), v_own[:, tile], preferred_element_type=F32)
        widest[i] = jnp.full(widest.shape[1:], MASKED, F32)

    lax.fori_loop(1, me + 1, gauge, 0)

    @pl.when(me > 0)
    def _():
        for i in range(pairs):
            old = peak[i]
            top = jnp.maximum(old, jnp.max(widest[i], axis=1, keepdims=True))
            factor = jnp.exp(old - top)
            peak[i] = top
            total[i] = total[i] * factor
            summed[i] = summed[i] * factor

    def attend(step, _):
        d = jnp.where(me == devices - 1, step, me + 1 - step)
        for i in range(pairs):
            weights = jnp.exp(raw[d - 1, i] - peak[i, :, :picked])
            total[i, :, :picked] += weights
            weigh[i] = weights.astype(BF16)
        arrived(1, d)
        for i in range(pairs):
            tile = slice(i * LANES, (i + 1) * LANES)
            summed[i] += jnp.dot(weigh[i], v_rows[d, :, tile], preferred_element_type=F32)
        return 0

    lax.fori_loop(1, me + 1, attend, 0)

    att_copies = []
    for i in range(pairs):
        ratio = summed[i] / jnp.sum(total[i], axis=1, keepdims=True)
        att_own[i] = jnp.where(lane < HEAD_DIM, ratio[:rows], ratio[rows:]).astype(BF16)
        att_copies.append(
            pltpu.make_async_remote_copy(
                src_ref=att_own.at[i], dst_ref=att_peer.at[i], send_sem=att_sem.at[0, i],
                recv_sem=att_sem.at[1, i], device_id={"tp": other}, device_id_type=MESH,
            )
        )
        att_copies[-1].start()
    wo_load.wait()
    own_rows = pl.ds(pl.multiple_of(core * head_width, head_width), head_width)
    peer_rows = pl.ds(pl.multiple_of(other * head_width, head_width), head_width)
    joined = lambda ref: jnp.concatenate([ref[i] for i in range(pairs)], axis=1)
    mixed = jnp.dot(joined(att_own), wo[own_rows, :], preferred_element_type=F32)
    for copy in att_copies:
        copy.wait_recv()
    mixed = mixed + jnp.dot(joined(att_peer), wo[peer_rows, :], preferred_element_type=F32)
    out_ref[...] = mixed.astype(BF16)

    for copy in att_copies:
        copy.wait_send()
    tok_copy.wait_send()

    def drain_list(d, _):
        list_copy(d, me - d).wait_send()
        return 0

    lax.fori_loop(1, me + 1, drain_list, 0)

    def drain_rows(d, _):
        each(row_copy(0, d, me + d, me), lambda c: c.wait_send())
        each(row_copy(1, d, me + d, me), lambda c: c.wait_send())
        return 0

    lax.fori_loop(1, devices - me, drain_rows, 0)

    @pl.when(me == 0)
    def _():
        def drain_root(d, _):
            root_copy(0, d).wait_send()
            root_copy(1, d).wait_send()
            return 0

        lax.fori_loop(1, devices, drain_root, 0)


def on_device(devices, tokens, query_weight, key_weight, value_weight, out_weight, chosen):
    rows, half = tokens.shape
    width, head_width = query_weight.shape
    pairs = head_width // LANES
    picked = CAP * BLOCK
    row_table, base_table = rotary_tables(rows, devices)
    vmem = pl.BlockSpec(memory_space=pltpu.VMEM)
    anywhere = pl.BlockSpec(memory_space=pl.ANY)
    dma = pltpu.SemaphoreType.DMA
    return pl.pallas_call(
        functools.partial(layer, devices),
        out_shape=pltpu.VMEM((rows, out_weight.shape[1]), BF16),
        in_specs=[anywhere] * 8,
        out_specs=vmem,
        scratch_shapes=[
            pltpu.VMEM(chosen.shape, jnp.int32),
            pltpu.VMEM(base_table.shape, F32),
            pltpu.VMEM((rows, 2 * LANES), F32),
            pltpu.VMEM((rows, half), BF16),
            pltpu.VMEM((rows, half), BF16),
            pltpu.VMEM((width, head_width), BF16),
            pltpu.VMEM((width, head_width), BF16),
            pltpu.VMEM((width, head_width), BF16),
            pltpu.VMEM(out_weight.shape, BF16),
            pltpu.VMEM((rows, head_width), F32),
            pltpu.VMEM((rows, head_width), F32),
            pltpu.VMEM((rows, head_width), F32),
            pltpu.VMEM((rows, head_width), BF16),
            pltpu.VMEM((rows, head_width), BF16),
            pltpu.VMEM((pairs, 2 * rows, LANES), BF16),
            pltpu.VMEM((devices,) + chosen.shape, jnp.int32),
            pltpu.VMEM((devices, picked, rows), BF16),
            pltpu.VMEM((devices, picked, head_width), BF16),
            pltpu.VMEM((devices, picked, head_width), BF16),
            pltpu.VMEM((devices - 1, pairs, 2 * rows, picked), F32),
            pltpu.VMEM((pairs, 2 * rows, picked), F32),
            pltpu.VMEM((pairs, 2 * rows, LANES), F32),
            pltpu.VMEM((pairs, 2 * rows, LANES), F32),
            pltpu.VMEM((pairs, 2 * rows, LANES), F32),
            pltpu.VMEM((pairs, 2 * rows, picked), BF16),
            pltpu.VMEM((pairs, rows, LANES), BF16),
            pltpu.VMEM((pairs, rows, LANES), BF16),
            dma((8,)),
            dma((2,)),
            dma((2, pairs)),
            dma((devices,)),
            dma((devices,)),
            dma((2, devices)),
            dma((2, devices)),
            dma((2, devices)),
            dma((2,)),
        ],
        compiler_params=pltpu.CompilerParams(
            collective_id=0, has_side_effects=True, vmem_limit_bytes=62 * 1024 * 1024
        ),
        name="layer",
    )(
        chosen, jnp.asarray(base_table), jnp.asarray(row_table), tokens,
        query_weight, key_weight, value_weight, out_weight,
    )


def solution(mesh):
    placed = (
        P(("dp", "kv"), "tp"),
        P(None, "tp"),
        P(None, "tp"),
        P(None, "tp"),
        P(None, "tp"),
        P(("dp", "kv"), None),
    )
    return jax.shard_map(
        functools.partial(on_device, mesh.shape["kv"]),
        mesh=mesh, in_specs=placed, out_specs=P(("dp", "kv"), "tp"), check_vma=False,
    )
```

```python
import functools

import jax
import jax.numpy as jnp
import numpy as np
from jax import lax
from jax.experimental import pallas as pl
from jax.experimental.pallas import tpu as pltpu
from jax.sharding import PartitionSpec as P

HEAD_DIM = 64
BLOCK = 32
CAP = 3
LANES = 128
ROTARY_BASE = 500000.0
MASKED = -1e30
MESH = pl.DeviceIdType.MESH
F32 = jnp.float32
BF16 = jnp.bfloat16


def rotary_tables(rows, devices):
    half = HEAD_DIM // 2
    inverse = (1.0 / ROTARY_BASE ** (np.arange(half, dtype=np.float64) / half))
    lanes = np.tile(inverse, LANES // half)[None, :]
    row_angle = np.arange(rows, dtype=np.float64)[:, None] * lanes
    base_angle = (np.arange(devices, dtype=np.float64) * rows)[:, None] * lanes
    pack = lambda a: np.concatenate([np.cos(a), np.sin(a)], axis=1).astype(np.float32)
    return pack(row_angle), pack(base_angle)


def listed_columns(chosen, holder, rows):
    blocks = rows // BLOCK
    ids = holder * blocks + lax.broadcasted_iota(jnp.int32, (blocks, rows), 1) // BLOCK
    hit = jnp.zeros((blocks, rows), F32)
    for slot in range(chosen.shape[1]):
        hit = jnp.where(chosen[:, slot : slot + 1] == ids, 1.0, hit)
    return hit


def selection(hit, earlier):
    blocks, rows = hit.shape
    need = jnp.broadcast_to(jnp.max(hit, axis=0, keepdims=True), hit.shape)
    rank = jnp.dot(need.astype(BF16), earlier, preferred_element_type=F32)
    shape = (CAP * BLOCK, rows)
    slot_row = lax.broadcasted_iota(jnp.int32, shape, 0)
    column = lax.broadcasted_iota(jnp.int32, shape, 1)
    wanted = (slot_row // BLOCK).astype(F32)
    place = jnp.where(need[:1] > 0.5, rank[:1], -1.0)
    same = (slot_row % BLOCK) == (column % BLOCK)
    return jnp.where(same & (place == wanted), 1.0, 0.0).astype(BF16)


def layer(
    devices,
    chosen_hbm, base_hbm, row_hbm, tok_hbm, wq_hbm, wk_hbm, wv_hbm, wo_hbm,
    out_ref,
    chosen_ref, base_ref, tab, tok_own, tok_peer, wq, wk, wv, wo, q_acc, k_acc, v_acc, k_own, v_own, q2,
    lists, picks, k_rows, v_rows, raw, widest, peak, total, summed, weigh, att_own, att_peer,
    load_sem, tok_sem, att_sem, list_send, list_recv, key_send, key_recv, root_send, root_recv,
):
    me = lax.axis_index("kv")
    core = lax.axis_index("tp")
    rows, half = tok_own.shape
    head_width = k_own.shape[1]
    pairs = head_width // LANES
    picked = CAP * BLOCK
    other = 1 - core

    loads = [
        pltpu.make_async_copy(src, dst, load_sem.at[i])
        for i, (src, dst) in enumerate(
            ((chosen_hbm, chosen_ref), (base_hbm, base_ref), (tok_hbm, tok_own), (wk_hbm, wk), (row_hbm, tab), (wv_hbm, wv), (wq_hbm, wq), (wo_hbm, wo))
        )
    ]
    for load in loads:
        load.start()
    chosen_load, base_load, tok_load, wk_load, tab_load, wv_load, wq_load, wo_load = loads

    barrier = pltpu.get_barrier_semaphore()
    pl.semaphore_signal(barrier, inc=1, device_id={"tp": other}, device_id_type=MESH)

    def greet(d, _):
        pl.semaphore_signal(
            barrier, inc=1, device_id={"kv": lax.rem(me + d, devices)}, device_id_type=MESH
        )
        return 0

    lax.fori_loop(1, devices, greet, 0)

    own_half = pl.ds(pl.multiple_of(core * half, half), half)
    peer_half = pl.ds(pl.multiple_of(other * half, half), half)

    tok_load.wait()
    wk_load.wait()
    k_acc[...] = jnp.dot(tok_own[...], wk[own_half, :], preferred_element_type=F32)

    pl.semaphore_wait(barrier, devices)

    def list_copy(d, target):
        return pltpu.make_async_remote_copy(
            src_ref=chosen_ref, dst_ref=lists.at[d], send_sem=list_send.at[d],
            recv_sem=list_recv.at[d], device_id={"kv": target}, device_id_type=MESH,
        )

    def send_list(d, _):
        list_copy(d, me - d).start()
        return 0

    chosen_load.wait()
    lax.fori_loop(1, me + 1, send_list, 0)
    tok_copy = pltpu.make_async_remote_copy(
        src_ref=tok_own, dst_ref=tok_peer, send_sem=tok_sem.at[0], recv_sem=tok_sem.at[1],
        device_id={"tp": other}, device_id_type=MESH,
    )
    tok_copy.start()

    wv_load.wait()
    v_acc[...] = jnp.dot(tok_own[...], wv[own_half, :], preferred_element_type=F32)
    wq_load.wait()
    q_acc[...] = jnp.dot(tok_own[...], wq[own_half, :], preferred_element_type=F32)

    tab_load.wait()
    base_load.wait()
    lane = lax.broadcasted_iota(jnp.int32, (rows, LANES), 1)
    first = (lane % HEAD_DIM) < HEAD_DIM // 2
    base = base_ref[pl.ds(me, 1), :]
    row_cos, row_sin = tab[:, :LANES], tab[:, LANES:]
    base_cos, base_sin = base[:, :LANES], base[:, LANES:]
    cosine = row_cos * base_cos - row_sin * base_sin
    sine = row_sin * base_cos + row_cos * base_sin
    sine = jnp.where(first, -sine, sine)
    tab[:, :LANES] = cosine
    tab[:, LANES:] = sine

    def rotated(x):
        swapped = jnp.where(
            first,
            pltpu.roll(x, LANES - HEAD_DIM // 2, axis=1),
            pltpu.roll(x, HEAD_DIM // 2, axis=1),
        )
        return x * tab[:, :LANES] + swapped * tab[:, LANES:]

    row_i = lax.broadcasted_iota(jnp.int32, (rows, rows), 0)
    col_i = lax.broadcasted_iota(jnp.int32, (rows, rows), 1)
    earlier = jnp.where((row_i % BLOCK == 0) & (row_i // BLOCK < col_i // BLOCK), 1.0, 0.0).astype(BF16)

    tok_copy.wait_recv()
    k_full = k_acc[...] + jnp.dot(tok_peer[...], wk[peer_half, :], preferred_element_type=F32)
    for i in range(pairs):
        tile = slice(i * LANES, (i + 1) * LANES)
        k_own[:, tile] = rotated(k_full[:, tile]).astype(BF16)

    buffers = ((k_own, k_rows), (v_own, v_rows))

    def row_copy(kind, d, target, holder):
        buffer = buffers[kind][1]

        def part(span):
            return pltpu.make_async_remote_copy(
                src_ref=buffer.at[lax.rem(me + d, devices), span], dst_ref=buffer.at[d, span],
                send_sem=key_send.at[kind, d], recv_sem=key_recv.at[kind, d],
                device_id={"kv": target}, device_id_type=MESH,
            )

        return part(slice(BLOCK, picked)), part(slice(0, picked)), holder == 0

    def each(copies, act):
        short, whole, is_short = copies
        pl.when(is_short)(lambda: act(short))
        pl.when(jnp.logical_not(is_short))(lambda: act(whole))

    relayed = devices > 2
    direct = devices - 2 if relayed else devices - 1
    relay_here = (me == devices - 2) if relayed else False

    def root_copy(kind, d, passing=False):
        own, buffer = buffers[kind]
        block = slice(0, BLOCK)
        return pltpu.make_async_remote_copy(
            src_ref=buffer.at[me, block] if passing else own.at[block], dst_ref=buffer.at[d, block],
            send_sem=root_send.at[kind, d], recv_sem=root_recv.at[kind],
            device_id={"kv": lax.rem(d, devices)}, device_id_type=MESH,
        )

    def send_root(kind):
        @pl.when(me == 0)
        def _():
            def one(step, _):
                root_copy(kind, direct - step).start()
                return 0

            lax.fori_loop(0, direct, one, 0)

    def arrived(kind, d):
        each(row_copy(kind, d, me, me - d), lambda c: c.wait_recv())

        @pl.when((d == me) & jnp.logical_not(relay_here))
        def _():
            root_copy(kind, d).wait_recv()

    send_root(0)

    def send_keys(d, _):
        list_copy(d, me).wait_recv()
        pick = selection(listed_columns(lists[d], me, rows), earlier)
        picks[d] = pick
        k_rows[me + d] = jnp.dot(pick, k_own[...], preferred_element_type=F32).astype(BF16)
        each(row_copy(0, d, me + d, me), lambda c: c.start())
        return 0

    lax.fori_loop(1, devices - me, send_keys, 0)

    v_own[...] = (
        v_acc[...] + jnp.dot(tok_peer[...], wv[peer_half, :], preferred_element_type=F32)
    ).astype(BF16)

    send_root(1)

    def send_values(step, _):
        d = devices - 1 - me - step
        v_rows[me + d] = jnp.dot(picks[d], v_own[...], preferred_element_type=F32).astype(BF16)
        each(row_copy(1, d, me + d, me), lambda c: c.start())
        return 0

    lax.fori_loop(0, devices - 1 - me, send_values, 0)

    q_full = q_acc[...] + jnp.dot(tok_peer[...], wq[peer_half, :], preferred_element_type=F32)
    for i in range(pairs):
        tile = slice(i * LANES, (i + 1) * LANES)
        q = rotated(q_full[:, tile]).astype(BF16).astype(F32) * (HEAD_DIM**-0.5)
        q2[i, :rows, :] = jnp.where(lane < HEAD_DIM, q, 0.0).astype(BF16)
        q2[i, rows:, :] = jnp.where(lane < HEAD_DIM, 0.0, q).astype(BF16)

    chosen = chosen_ref[...]

    def spread(hit):
        keys = hit.shape[1]
        blocks = hit.shape[0]
        wide = jnp.broadcast_to(hit[:, None, :], (blocks, BLOCK, keys))
        return wide.reshape(blocks * BLOCK, keys)

    def scores_of(i, keys):
        return lax.dot_general(
            q2[i], keys, (((1,), (1,)), ((), ())), preferred_element_type=F32
        )

    def gauge(d, _):
        hit = listed_columns(chosen, me - d, rows)
        pick = selection(hit, earlier)
        got = lax.dot_general(
            hit.astype(BF16), pick, (((1,), (1,)), ((), ())), preferred_element_type=F32
        )
        far = jnp.where(spread(got) > 0.5, 0.0, MASKED)
        far = jnp.concatenate([far, far], axis=0)
        arrived(0, d)
        for i in range(pairs):
            tile = slice(i * LANES, (i + 1) * LANES)
            scores = scores_of(i, k_rows[d, :, tile]) + far
            raw[d - 1, i] = scores
            widest[i] = jnp.maximum(widest[i], scores)
        return 0

    listed = spread(listed_columns(chosen, me, rows))
    bias = jnp.where((listed > 0.5) & (col_i <= row_i), 0.0, MASKED)
    bias = jnp.concatenate([bias, bias], axis=0)
    for i in range(pairs):
        tile = slice(i * LANES, (i + 1) * LANES)
        scores = scores_of(i, k_own[:, tile]) + bias
        top = jnp.max(scores, axis=1, keepdims=True)
        weights = jnp.exp(scores - top)
        peak[i] = jnp.broadcast_to(top, peak.shape[1:])
        total[i] = sum(weights[:, j : j + LANES] for j in range(0, rows, LANES))
        summed[i] = jnp.dot(weights.astype(BF16), v_own[:, tile], preferred_element_type=F32)
        widest[i] = jnp.full(widest.shape[1:], MASKED, F32)

    if relayed:

        @pl.when(relay_here)
        def _():
            for kind in range(2):
                root_copy(kind, me).wait_recv()
                root_copy(kind, devices - 1, True).start()

    lax.fori_loop(1, me + 1, gauge, 0)

    @pl.when(me > 0)
    def _():
        for i in range(pairs):
            old = peak[i]
            top = jnp.maximum(old, jnp.max(widest[i], axis=1, keepdims=True))
            factor = jnp.exp(old - top)
            peak[i] = top
            total[i] = total[i] * factor
            summed[i] = summed[i] * factor

    def attend(step, _):
        d = jnp.where(me == devices - 1, step, me + 1 - step)
        for i in range(pairs):
            weights = jnp.exp(raw[d - 1, i] - peak[i, :, :picked])
            total[i, :, :picked] += weights
            weigh[i] = weights.astype(BF16)
        arrived(1, d)
        for i in range(pairs):
            tile = slice(i * LANES, (i + 1) * LANES)
            summed[i] += jnp.dot(weigh[i], v_rows[d, :, tile], preferred_element_type=F32)
        return 0

    lax.fori_loop(1, me + 1, attend, 0)

    att_copies = []
    for i in range(pairs):
        ratio = summed[i] / jnp.sum(total[i], axis=1, keepdims=True)
        att_own[i] = jnp.where(lane < HEAD_DIM, ratio[:rows], ratio[rows:]).astype(BF16)
        att_copies.append(
            pltpu.make_async_remote_copy(
                src_ref=att_own.at[i], dst_ref=att_peer.at[i], send_sem=att_sem.at[0, i],
                recv_sem=att_sem.at[1, i], device_id={"tp": other}, device_id_type=MESH,
            )
        )
        att_copies[-1].start()
    wo_load.wait()
    own_rows = pl.ds(pl.multiple_of(core * head_width, head_width), head_width)
    peer_rows = pl.ds(pl.multiple_of(other * head_width, head_width), head_width)
    joined = lambda ref: jnp.concatenate([ref[i] for i in range(pairs)], axis=1)
    mixed = jnp.dot(joined(att_own), wo[own_rows, :], preferred_element_type=F32)
    for copy in att_copies:
        copy.wait_recv()
    mixed = mixed + jnp.dot(joined(att_peer), wo[peer_rows, :], preferred_element_type=F32)
    out_ref[...] = mixed.astype(BF16)

    for copy in att_copies:
        copy.wait_send()
    tok_copy.wait_send()

    def drain_list(d, _):
        list_copy(d, me - d).wait_send()
        return 0

    lax.fori_loop(1, me + 1, drain_list, 0)

    def drain_rows(d, _):
        each(row_copy(0, d, me + d, me), lambda c: c.wait_send())
        each(row_copy(1, d, me + d, me), lambda c: c.wait_send())
        return 0

    lax.fori_loop(1, devices - me, drain_rows, 0)

    @pl.when(me == 0)
    def _():
        def drain_root(d, _):
            root_copy(0, d).wait_send()
            root_copy(1, d).wait_send()
            return 0

        lax.fori_loop(1, direct + 1, drain_root, 0)

    if relayed:

        @pl.when(relay_here)
        def _():
            for kind in range(2):
                root_copy(kind, devices - 1, True).wait_send()


def on_device(devices, tokens, query_weight, key_weight, value_weight, out_weight, chosen):
    rows, half = tokens.shape
    width, head_width = query_weight.shape
    pairs = head_width // LANES
    picked = CAP * BLOCK
    row_table, base_table = rotary_tables(rows, devices)
    vmem = pl.BlockSpec(memory_space=pltpu.VMEM)
    anywhere = pl.BlockSpec(memory_space=pl.ANY)
    dma = pltpu.SemaphoreType.DMA
    return pl.pallas_call(
        functools.partial(layer, devices),
        out_shape=pltpu.VMEM((rows, out_weight.shape[1]), BF16),
        in_specs=[anywhere] * 8,
        out_specs=vmem,
        scratch_shapes=[
            pltpu.VMEM(chosen.shape, jnp.int32),
            pltpu.VMEM(base_table.shape, F32),
            pltpu.VMEM((rows, 2 * LANES), F32),
            pltpu.VMEM((rows, half), BF16),
            pltpu.VMEM((rows, half), BF16),
            pltpu.VMEM((width, head_width), BF16),
            pltpu.VMEM((width, head_width), BF16),
            pltpu.VMEM((width, head_width), BF16),
            pltpu.VMEM(out_weight.shape, BF16),
            pltpu.VMEM((rows, head_width), F32),
            pltpu.VMEM((rows, head_width), F32),
            pltpu.VMEM((rows, head_width), F32),
            pltpu.VMEM((rows, head_width), BF16),
            pltpu.VMEM((rows, head_width), BF16),
            pltpu.VMEM((pairs, 2 * rows, LANES), BF16),
            pltpu.VMEM((devices,) + chosen.shape, jnp.int32),
            pltpu.VMEM((devices, picked, rows), BF16),
            pltpu.VMEM((devices, picked, head_width), BF16),
            pltpu.VMEM((devices, picked, head_width), BF16),
            pltpu.VMEM((devices - 1, pairs, 2 * rows, picked), F32),
            pltpu.VMEM((pairs, 2 * rows, picked), F32),
            pltpu.VMEM((pairs, 2 * rows, LANES), F32),
            pltpu.VMEM((pairs, 2 * rows, LANES), F32),
            pltpu.VMEM((pairs, 2 * rows, LANES), F32),
            pltpu.VMEM((pairs, 2 * rows, picked), BF16),
            pltpu.VMEM((pairs, rows, LANES), BF16),
            pltpu.VMEM((pairs, rows, LANES), BF16),
            dma((8,)),
            dma((2,)),
            dma((2, pairs)),
            dma((devices,)),
            dma((devices,)),
            dma((2, devices)),
            dma((2, devices)),
            dma((2, devices)),
            dma((2,)),
        ],
        compiler_params=pltpu.CompilerParams(
            collective_id=0, has_side_effects=True, vmem_limit_bytes=62 * 1024 * 1024
        ),
        name="layer",
    )(
        chosen, jnp.asarray(base_table), jnp.asarray(row_table), tokens,
        query_weight, key_weight, value_weight, out_weight,
    )


def solution(mesh):
    placed = (
        P(("dp", "kv"), "tp"),
        P(None, "tp"),
        P(None, "tp"),
        P(None, "tp"),
        P(None, "tp"),
        P(("dp", "kv"), None),
    )
    return jax.shard_map(
        functools.partial(on_device, mesh.shape["kv"]),
        mesh=mesh, in_specs=placed, out_specs=P(("dp", "kv"), "tp"), check_vma=False,
    )
```
